32 devices in a mesh: sp: 16 (over z, y, x), tp: 2 (over core).
Axes of the slice: x: 2, y: 2, z: 4, core: 2. Of those that a mesh axis runs over, the one named last changes fastest.
Arguments:
- residual_in: bfloat16 [6144, 2048], P(('sp', 'tp')), may hold values from -6 to 6
- conv_values: bfloat16 [6144, 1024], P('sp', 'tp'), may hold values from -60 to 60
- conv_gates: bfloat16 [6144, 1024], P('sp', 'tp'), may hold values from -8 to 8
- conv_kernel: float32 [31, 1024], P(None, 'tp'), may hold values from -1 to 1
- conv_bias: float32 [1024], P('tp'), may hold values from -3 to 3
- chan_gain: float32 [1024], P('tp'), may hold values from 0.1 to 1.9
- chan_shift: float32 [1024], P('tp'), may hold values from -3 to 3
- out_weight: bfloat16 [1024, 2048], replicated, may hold values from -0.1875 to 0.1875
- norm_gain: float32 [2048], replicated, may hold values from 0.1 to 1.9
- route_ids: int32 [6144, 2], P(('sp', 'tp')), may hold values from 0 to 15, all different within a row; in each aligned block of 192 rows (0 to 191, 192 to 383, ...) at most 48 rows name the same one
- route_weights: float32 [6144, 2], P(('sp', 'tp')), may hold values from 0.25 to 1.5
- expert_gate: bfloat16 [16, 2048, 2048], P('sp', None, 'tp'), may hold values from -0.125 to 0.125
- expert_up: bfloat16 [16, 2048, 2048], P('sp', None, 'tp'), may hold values from -0.125 to 0.125
- expert_down: bfloat16 [16, 2048, 2048], P('sp', 'tp'), may hold values from -0.125 to 0.125
Outputs:
- layer_out: bfloat16 [6144, 2048], P(('sp', 'tp'))
The draws below stay inside these ranges and needn't reach their ends.
Inputs may be any that keep to these rules, and one draw needn't show every extreme that they name: `route_ids`: each row names 2 different experts. Among the rows of one device (aligned blocks of 192 rows) no expert is named by more than 48 rows, a bound that some block reaches.
All inputs are finite; a program needn't handle non-finite values.
Results may differ from the reference program's by a relative error of at most 0.014.
Values may be sent and summed in bfloat16 or wider, within the bound.
No kernel may reach another device: no remote copies, remote signals or barrier semaphores. Data moves between devices by JAX's collectives and lax.ppermute only.
A program may use at most 128 MiB of HBM per device.

```python
import math
import jax
import jax.numpy as jnp
import numpy as np
from jax import lax

D = 2048
C = 1024
FF = 2048
KW = 31
TOPK = 2
ROWS = 192
TOKENS = 6144
EXPERTS = 16
CAP = 48
N_SP = 16
N_TP = 2


def draw_conv_values(key, part):
    keys = jax.random.split(jax.random.fold_in(key, 11), 3)
    columns = jnp.exp(jax.random.uniform(keys[0], (C,), jnp.float32, 0.0, math.log(10.0)))
    rowscale = jnp.exp(jax.random.uniform(keys[1], (TOKENS, 1), jnp.float32, 0.0, math.log(4.0)))
    base = jnp.clip(jax.random.normal(keys[2], (TOKENS, C), jnp.float32), -4.0, 4.0)
    values = jnp.clip(base * columns[None, :] * rowscale * 0.4, -60.0, 60.0)
    return values.astype(jnp.bfloat16)


def level_of(own_key, shape, pieces, smallest, high):
    def one(dim, blocks):
        draws = jax.random.uniform(jax.random.fold_in(jax.random.fold_in(own_key, 6), dim), (blocks,), jnp.float32, smallest / len(pieces), high / len(pieces))
        return jnp.repeat(jnp.exp(draws), shape[dim] // blocks).reshape((-1,) + (1,) * (len(shape) - dim - 1))

    level = one(*pieces[0])
    for cut in pieces[1:]:
        level = level * one(*cut)
    return level


def shared_out(rng, own, number, rows, amount, top, bound, lean):
    order = jax.random.permutation(rng, amount)
    packed, ordinary = portions_of(amount, rows * top, bound, lean, True), portions_of(amount, rows * top, bound, lean, False)
    places = jnp.arange(amount)

    def named(sizes, turn):
        used = int((sizes > 0).sum())
        fixed = max(1, used // 4)
        shifted = fixed + (places - fixed + turn * (used - fixed)) % max(1, amount - fixed)
        return jnp.zeros((amount,), jnp.int32).at[order[jnp.where(places < fixed, places, shifted)]].set(jnp.asarray(sizes, jnp.int32))

    sizes = jnp.where(number % 4 == 0, named(packed, number // 4), named(ordinary, number - number // 4 - 1))
    mixed = jax.random.permutation(jax.random.fold_in(own, 3), amount)
    giver, sink = mixed[0:amount // 2 * 2:2], mixed[1:amount // 2 * 2:2]
    margin = jnp.minimum(sizes[giver] - 1, bound - sizes[sink]) // 2
    margin = jnp.where((giver == order[0]) | (sink == order[0]) | (sizes[sink] == 0), 0, jnp.maximum(margin, 0))
    shifted = jax.random.randint(jax.random.fold_in(own, 4), (amount // 2,), 0, 1 << 20) % (margin + 1)
    sizes = sizes.at[giver].add(-shifted).at[sink].add(shifted)
    items = jnp.searchsorted(jnp.cumsum(sizes), jnp.arange(rows * top), side="right").astype(jnp.int32)
    grid = items.reshape(top, rows).T
    grid = grid[jax.random.permutation(jax.random.fold_in(own, 1), rows)]
    turn = jax.random.randint(jax.random.fold_in(own, 2), (rows, 1), 0, top)
    return jnp.take_along_axis(grid, (jnp.arange(top)[None, :] + turn) % top, axis=1)


def portions_of(number_of, total, bound, lean, full):
    loads = [(1 << 20) // math.isqrt(grade ** lean) + 1 for grade in range(1, number_of + 1)]
    largest = bound if full else min(bound, max(-(-total // number_of), total * loads[0] // sum(loads)))
    least = 1 if total - largest >= number_of - 1 else 0
    counts, spare = [largest] + [least] * (number_of - 1), total - largest - least * (number_of - 1)
    while spare > 0:
        movable = [i for i in range(1, number_of) if counts[i] < largest] or [i for i in range(1, number_of) if counts[i] < bound]
        pool, budget = sum([loads[i] for i in movable]), spare
        for i in movable:
            more = min(bound - counts[i], max(1, budget * loads[i] // pool), spare)
            counts[i] = counts[i] + more
            spare = spare - more
    return np.array(counts)


def centred(own_key, shape, deviation, most, pieces=(), held_as=jnp.bfloat16):
    loudness = level_of(own_key, shape, pieces, -0.22, 0.18) if pieces else 1.0
    result = jax.random.normal(own_key, shape, jnp.float32) * deviation * loudness
    return jnp.minimum(jnp.maximum(result, -most), most).astype(held_as)


def setup_inputs(seed: int = 0) -> dict:
    seeds = jax.random.split(jax.random.key(seed), 15)
    residual_in = centred(seeds[0], (TOKENS, D), 1.0, 6.0, ((0, 32),))
    conv_values = draw_conv_values(jax.random.fold_in(seeds[14], 71), 0)
    conv_gates = centred(seeds[2], (TOKENS, C), 1.5, 8.0, ((0, 16), (1, 2)))
    conv_kernel = centred(seeds[3], (KW, C), KW ** -0.5, 1.0, ((1, 2),), jnp.float32)
    conv_bias = centred(seeds[4], (C,), 0.5, 3.0, ((0, 2),), jnp.float32)
    chan_gain = jnp.clip(1.0 + 0.18 * jax.random.normal(seeds[5], (C,), jnp.float32), 0.1, 1.9)
    chan_shift = centred(seeds[6], (C,), 0.5, 3.0, ((0, 2),), jnp.float32)
    out_weight = centred(seeds[7], (C, D), C ** -0.5, 0.1875)
    norm_gain = jnp.clip(1.0 + 0.18 * jax.random.normal(seeds[8], (D,), jnp.float32), 0.1, 1.9)
    route_ids_keys = jax.random.split(jax.random.fold_in(seeds[9], 1), TOKENS // ROWS)
    route_ids_turns = jax.random.permutation(jax.random.fold_in(seeds[9], 3), TOKENS // ROWS)
    route_ids = jax.vmap(lambda own, number: shared_out(jax.random.fold_in(seeds[9], 2), own, number, ROWS, EXPERTS, TOPK, CAP, 2))(route_ids_keys, route_ids_turns).reshape((TOKENS, TOPK))
    route_weights = jnp.clip(0.25 + 1.25 * jax.random.uniform(seeds[10], (TOKENS, TOPK), jnp.float32) ** level_of(seeds[10], (TOKENS, TOPK), ((0, 32),), -0.2, 0.2), 0.25, 1.5)
    expert_gate = centred(seeds[11], (EXPERTS, D, FF), D ** -0.5, 0.125, ((0, 16), (2, 2)))
    expert_up = centred(seeds[12], (EXPERTS, D, FF), D ** -0.5, 0.125, ((0, 16), (2, 2)))
    expert_down = centred(seeds[13], (EXPERTS, FF, D), FF ** -0.5, 0.125, ((0, 16), (1, 2)))
    return {"residual_in": residual_in, "conv_values": conv_values, "conv_gates": conv_gates, "conv_kernel": conv_kernel, "conv_bias": conv_bias, "chan_gain": chan_gain, "chan_shift": chan_shift, "out_weight": out_weight, "norm_gain": norm_gain, "route_ids": route_ids, "route_weights": route_weights, "expert_gate": expert_gate, "expert_up": expert_up, "expert_down": expert_down}


def reference(residual_in, conv_values, conv_gates, conv_kernel, conv_bias, chan_gain, chan_shift, out_weight, norm_gain, route_ids, route_weights, expert_gate, expert_up, expert_down):
    seq_count = residual_in.shape[0]
    gated = (conv_values.astype(jnp.float32) * jax.nn.sigmoid(conv_gates.astype(jnp.float32))).astype(jnp.bfloat16)
    padded = jnp.concatenate([jnp.zeros((KW - 1, C), jnp.float32), gated.astype(jnp.float32)], 0)
    mixed = jnp.zeros((seq_count, C), jnp.float32) + conv_bias[None, :]
    for tap_index in range(KW):
        mixed = mixed + conv_kernel[tap_index][None, :] * padded[tap_index:tap_index + seq_count]
    center = lax.optimization_barrier(jnp.mean(mixed, 1, keepdims=True))
    spread = lax.optimization_barrier(jnp.mean(mixed * mixed, 1, keepdims=True)) - center * center
    normed = (mixed - center) * lax.rsqrt(spread + 1e-06) * chan_gain[None, :] + chan_shift[None, :]
    activated = jax.nn.silu(normed).astype(jnp.bfloat16)
    projected = jnp.dot(activated, out_weight, preferred_element_type=jnp.float32)
    after_mix = (residual_in.astype(jnp.float32) + projected).astype(jnp.bfloat16)
    after_f = after_mix.astype(jnp.float32)
    normal_rows = (after_f * lax.rsqrt(lax.optimization_barrier(jnp.mean(after_f * after_f, 1, keepdims=True)) + 1e-06) * norm_gain[None, :]).astype(jnp.bfloat16)
    flat_ids = route_ids.reshape(-1)
    flat_weights = route_weights.reshape(-1)
    most_rows = N_SP * N_TP * CAP
    half_width = FF // N_TP

    def per_expert(totals, inputs):
        gate_w, up_w, down_w, expert_index = inputs
        chosen = flat_ids == expert_index
        order = jnp.argsort(jnp.where(chosen, 0, 1).astype(jnp.int32), stable=True)[:most_rows].astype(jnp.int32)
        valid = chosen[order]
        token_index = (order // TOPK).astype(jnp.int32)
        picked = normal_rows[token_index]
        gate = jnp.dot(picked, gate_w, preferred_element_type=jnp.float32)
        upper = jnp.dot(picked, up_w, preferred_element_type=jnp.float32)
        hidden = (jax.nn.silu(gate) * upper).astype(jnp.bfloat16)
        summed = jnp.zeros((most_rows, D), jnp.float32)
        for half_index in range(N_TP):
            partial_out = jnp.dot(hidden[:, half_index * half_width:(half_index + 1) * half_width], down_w[half_index * half_width:(half_index + 1) * half_width], preferred_element_type=jnp.float32)
            partial_out = lax.optimization_barrier(partial_out.astype(jnp.bfloat16))
            summed = summed + partial_out.astype(jnp.float32)
        expert_out = summed.astype(jnp.bfloat16).astype(jnp.float32)
        weight = jnp.where(valid, flat_weights[order], 0.0)
        totals = totals.at[token_index].add(weight[:, None] * expert_out)
        return (totals, None)
    totals, unused = lax.scan(per_expert, jnp.zeros((seq_count, D), jnp.float32), (expert_gate, expert_up, expert_down, jnp.arange(EXPERTS, dtype=jnp.int32)))
    return (after_f + totals).astype(jnp.bfloat16)
```

```python
import jax
import jax.numpy as jnp
from jax import lax
from jax.sharding import PartitionSpec as P


def from_behind(value, axis, steps):
    count = lax.axis_size(axis)
    first, last = (max(0, -steps), min(count, count - steps))
    return lax.ppermute(value, axis, [(source, source + steps) for source in range(first, last)])


def on_device(
    residual_in,
    conv_values,
    conv_gates,
    conv_kernel,
    conv_bias,
    chan_gain,
    chan_shift,
    out_weight,
    norm_gain,
    route_ids,
    route_weights,
    expert_gate,
    expert_up,
    expert_down,
):
    taps_count = conv_kernel.shape[0]
    tok_count, local_chan = conv_values.shape
    tp_count = lax.axis_size("tp")
    all_chan = local_chan * tp_count
    gated = (
        conv_values.astype(jnp.float32) * jax.nn.sigmoid(conv_gates.astype(jnp.float32))
    ).astype(jnp.bfloat16)
    earlier = from_behind(gated[tok_count - (taps_count - 1) :], "sp", 1)
    extended = jnp.concatenate([earlier, gated], 0).astype(jnp.float32)
    mixed = jnp.zeros((tok_count, local_chan), jnp.float32) + conv_bias[None, :]
    for tap_index in range(taps_count):
        mixed = (
            mixed + conv_kernel[tap_index][None, :] * extended[tap_index : tap_index + tok_count]
        )
    row_total = jnp.sum(mixed, 1)
    row_square = jnp.sum(mixed * mixed, 1)
    row_total, row_square = lax.psum((row_total, row_square), "tp")
    center = (row_total / all_chan)[:, None]
    spread = (row_square / all_chan)[:, None] - center * center
    normed = (mixed - center) * lax.rsqrt(spread + 1e-06) * chan_gain[None, :] + chan_shift[None, :]
    activated = jax.nn.silu(normed).astype(jnp.bfloat16)
    row_count = tok_count // tp_count
    regrouped = lax.all_to_all(activated, "tp", split_axis=0, concat_axis=1, tiled=True)
    projected = jnp.dot(regrouped, out_weight, preferred_element_type=jnp.float32)
    after_f = (residual_in.astype(jnp.float32) + projected).astype(jnp.bfloat16).astype(jnp.float32)
    normal_rows = (
        after_f
        * lax.rsqrt(jnp.mean(after_f * after_f, 1, keepdims=True) + 1e-06)
        * norm_gain[None, :]
    ).astype(jnp.bfloat16)
    model_width = normal_rows.shape[1]
    experts_all = expert_gate.shape[0] * lax.axis_size("sp")
    choose_count = route_ids.shape[1]
    slot_cap = max(2, (2 * choose_count * row_count + experts_all - 1) // experts_all)
    onehot = (
        route_ids.reshape(-1)[:, None] == jnp.arange(experts_all, dtype=jnp.int32)[None, :]
    ).astype(jnp.int32)
    before = jnp.cumsum(onehot, 0) - onehot
    ranking = jnp.sum(before * onehot, 1).reshape(row_count, choose_count)
    slot_ids = route_ids * slot_cap + ranking
    positions = lax.broadcasted_iota(jnp.int32, (experts_all * slot_cap, 1, 1), 0)
    dispatch = jnp.any(positions == slot_ids[None, :, :], axis=2).astype(jnp.bfloat16)
    sendable = jnp.dot(dispatch, normal_rows, preferred_element_type=jnp.float32).astype(
        jnp.bfloat16
    )
    sendable = sendable.reshape(experts_all, slot_cap, model_width)
    received = lax.all_to_all(sendable, "sp", split_axis=0, concat_axis=0, tiled=True)
    flat_rows = received.reshape(experts_all * slot_cap, model_width)
    halves = [(expert_gate[0], expert_up[0], expert_down[0])]
    for shift in range(1, tp_count):
        turn = [(source, (source + shift) % tp_count) for source in range(tp_count)]
        halves.append(
            tuple(
                lax.ppermute(held[0], "tp", turn) for held in (expert_gate, expert_up, expert_down)
            )
        )
    total = 0.0
    for gate_w, up_w, down_w in halves:
        gate = jnp.dot(flat_rows, gate_w, preferred_element_type=jnp.float32)
        upper = jnp.dot(flat_rows, up_w, preferred_element_type=jnp.float32)
        hidden = (jax.nn.silu(gate) * upper).astype(jnp.bfloat16)
        total = total + jnp.dot(hidden, down_w, preferred_element_type=jnp.float32)
    summed = total.astype(jnp.bfloat16).reshape(experts_all, slot_cap, model_width)
    results = lax.all_to_all(summed, "sp", split_axis=0, concat_axis=0, tiled=True)
    flat_out = results.reshape(experts_all * slot_cap, model_width)
    slots = lax.broadcasted_iota(jnp.int32, (1, experts_all * slot_cap), 1)
    combined = after_f
    for choice in range(choose_count):
        chosen = (slots == slot_ids[:, choice : choice + 1]).astype(jnp.bfloat16)
        picked = jnp.dot(chosen, flat_out, preferred_element_type=jnp.float32)
        combined = combined + route_weights[:, choice : choice + 1] * picked
    return combined.astype(jnp.bfloat16)


def solution(mesh):
    placed = (
        P(("sp", "tp"), None),
        P("sp", "tp"),
        P("sp", "tp"),
        P(None, "tp"),
        P("tp"),
        P("tp"),
        P("tp"),
        P(),
        P(),
        P(("sp", "tp"), None),
        P(("sp", "tp"), None),
        P("sp", None, "tp"),
        P("sp", None, "tp"),
        P("sp", "tp", None),
    )
    return jax.shard_map(
        on_device, mesh=mesh, in_specs=placed, out_specs=P(("sp", "tp"), None), check_vma=False
    )
```

```python
import functools

import jax
import jax.numpy as jnp
from jax import lax
from jax.experimental import pallas as pl
from jax.experimental.pallas import tpu as pltpu
from jax.sharding import PartitionSpec as P


def expert_body(count, own_steps, rows, *refs):
    gates, uppers, downs = (refs[:count], refs[count : 2 * count], refs[2 * count : 3 * count])
    out, hidden = refs[3 * count :]
    step = pl.program_id(0)
    width = gates[0].shape[1]
    for part in range(count):

        @pl.when((step >= part * own_steps) & (step < (part + 1) * own_steps))
        def _(part=part):
            gate = jnp.dot(rows[...], gates[part][...], preferred_element_type=jnp.float32)
            upper = jnp.dot(rows[...], uppers[part][...], preferred_element_type=jnp.float32)
            value = (gate * jax.nn.sigmoid(gate) * upper).astype(jnp.bfloat16)
            hidden[step] = value

    @pl.when(step >= count * own_steps)
    def _():
        total = None
        for part in range(count):
            for piece in range(own_steps):
                product = jnp.dot(
                    hidden[part * own_steps + piece],
                    downs[part][piece * width : (piece + 1) * width, :],
                    preferred_element_type=jnp.float32,
                )
                total = product if total is None else total + product
        out[...] = total.astype(jnp.bfloat16)


def expert_call(rows, gates, uppers, downs):
    count = len(gates)
    row_total, model_width = rows.shape
    own_hidden = gates[0].shape[1]
    width = min(512, own_hidden)
    own_steps = own_hidden // width
    first_steps = count * own_steps
    out_steps = model_width // width

    def inward(part):
        return pl.BlockSpec(
            (model_width, width),
            lambda i: (0, jnp.clip(i - part * own_steps, 0, own_steps - 1)),
        )

    outward = pl.BlockSpec(
        (own_hidden, width), lambda i: (0, jnp.clip(i - first_steps, 0, out_steps - 1))
    )
    return pl.pallas_call(
        functools.partial(expert_body, count, own_steps),
        grid=(first_steps + out_steps,),
        in_specs=[pl.BlockSpec((row_total, model_width), lambda i: (0, 0))]
        + [inward(part) for part in range(count)] * 2
        + [outward] * count,
        out_specs=pl.BlockSpec(
            (row_total, width), lambda i: (0, jnp.clip(i - first_steps, 0, out_steps - 1))
        ),
        out_shape=jax.ShapeDtypeStruct((row_total, model_width), jnp.bfloat16),
        scratch_shapes=[pltpu.VMEM((first_steps, row_total, width), jnp.bfloat16)],
        compiler_params=pltpu.CompilerParams(dimension_semantics=("arbitrary",)),
        cost_estimate=pl.CostEstimate(
            flops=6 * row_total * model_width * own_hidden * count,
            bytes_accessed=6 * model_width * own_hidden * count,
            transcendentals=row_total * own_hidden * count,
        ),
        name="expert_rows",
    )(rows, *gates, *uppers, *downs)


def front_body(
    taps_count,
    extended,
    small,
    gain,
    residual_in,
    out_weight,
    after,
    normal,
    weight,
    residual,
    mixed,
    activated,
    arrivals,
):
    fetch_weight = pltpu.make_async_copy(out_weight, weight, arrivals.at[0])
    fetch_residual = pltpu.make_async_copy(residual_in, residual, arrivals.at[1])
    fetch_weight.start()
    fetch_residual.start()
    row_count, chan_count = mixed.shape
    model_width = after.shape[1]
    lanes = min(128, chan_count)
    piece = 32 if row_count % 32 == 0 else row_count

    def convolve(index, carry):
        here = pl.ds(pl.multiple_of(index * lanes, lanes), lanes)
        total = jnp.zeros((row_count, lanes), jnp.float32) + small[taps_count : taps_count + 1, here]
        for tap_index in range(taps_count):
            total = (
                total
                + small[tap_index : tap_index + 1, here]
                * extended[tap_index : tap_index + row_count, here]
            )
        mixed[:, here] = total
        return carry

    lax.fori_loop(0, chan_count // lanes, convolve, 0)
    scale = small[taps_count + 1 : taps_count + 2, :]
    shift = small[taps_count + 2 : taps_count + 3, :]

    def normalise(index, carry):
        here = pl.ds(pl.multiple_of(index * piece, piece), piece)
        values = mixed[here, :]
        center = jnp.sum(values, 1, keepdims=True) / chan_count
        spread = jnp.sum(values * values, 1, keepdims=True) / chan_count - center * center
        normed = (values - center) * lax.rsqrt(spread + 1e-06) * scale + shift
        activated[here, :] = (normed * jax.nn.sigmoid(normed)).astype(jnp.bfloat16)
        return carry

    lax.fori_loop(0, row_count // piece, normalise, 0)
    fetch_weight.wait()
    fetch_residual.wait()
    width = min(512, model_width)
    squares = jnp.zeros((row_count, 1), jnp.float32)
    for start in range(0, model_width, width):
        here = slice(start, start + width)
        product = jnp.dot(activated[...], weight[:, here], preferred_element_type=jnp.float32)
        rounded = (residual[:, here].astype(jnp.float32) + product).astype(jnp.bfloat16)
        after[:, here] = rounded
        again = rounded.astype(jnp.float32)
        squares = squares + jnp.sum(again * again, 1, keepdims=True)
    factor = lax.rsqrt(squares / model_width + 1e-06)
    for start in range(0, model_width, width):
        here = slice(start, start + width)
        value = after[:, here].astype(jnp.float32) * factor * gain[:, here]
        normal[:, here] = value.astype(jnp.bfloat16)


def front_call(taps_count, extended, small, gain, residual_in, out_weight):
    row_count, model_width = residual_in.shape
    chan_count = extended.shape[1]
    inside = pl.BlockSpec(memory_space=pltpu.VMEM)
    outside = pl.BlockSpec(memory_space=pl.ANY)
    result = jax.ShapeDtypeStruct((row_count, model_width), jnp.bfloat16)
    return pl.pallas_call(
        functools.partial(front_body, taps_count),
        in_specs=[inside, inside, inside, outside, outside],
        out_specs=[inside, inside],
        out_shape=[result, result],
        scratch_shapes=[
            pltpu.VMEM(out_weight.shape, jnp.bfloat16),
            pltpu.VMEM((row_count, model_width), jnp.bfloat16),
            pltpu.VMEM((row_count, chan_count), jnp.float32),
            pltpu.VMEM((row_count, chan_count), jnp.bfloat16),
            pltpu.SemaphoreType.DMA((2,)),
        ],
        cost_estimate=pl.CostEstimate(
            flops=2 * row_count * chan_count * (model_width + taps_count),
            bytes_accessed=2 * chan_count * model_width + 8 * row_count * model_width,
            transcendentals=row_count * chan_count,
        ),
        name="front_rows",
    )(extended, small, gain, residual_in, out_weight)


def on_device(
    residual_in,
    conv_values,
    conv_gates,
    conv_kernel,
    conv_bias,
    chan_gain,
    chan_shift,
    out_weight,
    norm_gain,
    route_ids,
    route_weights,
    expert_gate,
    expert_up,
    expert_down,
):
    taps_count = conv_kernel.shape[0]
    tok_count, local_chan = conv_values.shape
    tp_count = lax.axis_size("tp")
    row_count = tok_count // tp_count
    halo = taps_count - 1
    place = lax.axis_index("tp")
    sp_count = lax.axis_size("sp")
    gated = (
        conv_values.astype(jnp.float32) * jax.nn.sigmoid(conv_gates.astype(jnp.float32))
    ).astype(jnp.bfloat16)
    small = jnp.concatenate(
        [conv_kernel, conv_bias[None, :], chan_gain[None, :], chan_shift[None, :]], 0
    )
    padded = jnp.concatenate([jnp.zeros((halo, local_chan), jnp.bfloat16), gated], 0)

    def window(member):
        return lax.dynamic_slice_in_dim(padded, member * row_count, row_count + halo, 0)

    rows_by_source, small_by_source = ([window(place)], [small])
    for shift in range(1, tp_count):
        turn = [(source, (source + shift) % tp_count) for source in range(tp_count)]
        rows_by_source.append(lax.ppermute(window((place + shift) % tp_count), "tp", turn))
        small_by_source.append(lax.ppermute(small, "tp", turn))
    last = gated[tok_count - halo :]
    earlier = []
    for channel in range(tp_count):
        pairs = [
            (source * tp_count + channel, (source + 1) * tp_count) for source in range(sp_count - 1)
        ]
        earlier.append(lax.ppermute(last, ("sp", "tp"), pairs))

    def in_order(pieces):
        ordered = []
        for channel in range(tp_count):
            chosen = pieces[0]
            for shift in range(1, tp_count):
                chosen = jnp.where((place - shift) % tp_count == channel, pieces[shift], chosen)
            ordered.append(chosen)
        return ordered

    columns = []
    for rows, before_rows in zip(in_order(rows_by_source), earlier):
        first = rows[:halo].astype(jnp.float32) + before_rows.astype(jnp.float32)
        columns.append(jnp.concatenate([first, rows[halo:].astype(jnp.float32)], 0))
    extended = jnp.concatenate(columns, 1)
    after_mix, normal_rows = front_call(
        taps_count,
        extended,
        jnp.concatenate(in_order(small_by_source), 1),
        norm_gain[None, :],
        residual_in,
        out_weight,
    )
    after_f = after_mix.astype(jnp.float32)
    model_width = normal_rows.shape[1]
    experts_all = expert_gate.shape[0] * lax.axis_size("sp")
    choose_count = route_ids.shape[1]
    slot_cap = max(2, (2 * choose_count * row_count + experts_all - 1) // experts_all)
    onehot = (
        route_ids.reshape(-1)[:, None] == jnp.arange(experts_all, dtype=jnp.int32)[None, :]
    ).astype(jnp.int32)
    before = jnp.cumsum(onehot, 0) - onehot
    ranking = jnp.sum(before * onehot, 1).reshape(row_count, choose_count)
    slot_ids = route_ids * slot_cap + ranking
    half = sp_count // 2
    across = [(source, (source + half) % sp_count) for source in range(sp_count)]
    groups = [list(range(start, start + half)) for start in range(0, sp_count, half)]
    exchange = functools.partial(
        lax.all_to_all,
        axis_name="sp",
        split_axis=0,
        concat_axis=0,
        tiled=True,
        axis_index_groups=groups,
    )
    held = (expert_gate[0], expert_up[0], expert_down[0])
    weights = [held]
    for shift in range(1, tp_count):
        turn = [(source, (source + shift) % tp_count) for source in range(tp_count)]
        weights.append(tuple(lax.ppermute(piece, "tp", turn) for piece in held))
    gates, uppers, downs = zip(*weights)
    their_rows = lax.ppermute(normal_rows, "sp", across)
    packed = jnp.concatenate([slot_ids.astype(jnp.float32), route_weights], 1)
    packed, normal_rows = lax.optimization_barrier((packed, normal_rows))
    their_packed = lax.ppermute(packed, "sp", across)
    their_slots = their_packed[:, :choose_count].astype(jnp.int32)
    their_weights = their_packed[:, choose_count:]
    local = half * slot_cap
    base = (lax.axis_index("sp") // half) * local

    def sent_out(rows, slots):
        positions = base + lax.broadcasted_iota(jnp.int32, (local, 1, 1), 0)
        dispatch = jnp.any(positions == slots[None, :, :], axis=2).astype(jnp.bfloat16)
        sendable = jnp.dot(dispatch, rows, preferred_element_type=jnp.float32)
        return exchange(sendable.astype(jnp.bfloat16).reshape(half, slot_cap, model_width))

    def worked(rows):
        return expert_call(rows.reshape(local, model_width), gates, uppers, downs)

    def sent_back(rows):
        return exchange(rows.reshape(half, slot_cap, model_width)).reshape(local, model_width)

    def weighted(results, slots, scale):
        positions = base + lax.broadcasted_iota(jnp.int32, (1, local), 1)
        total = 0.0
        for choice in range(choose_count):
            chosen = (positions == slots[:, choice : choice + 1]).astype(jnp.bfloat16)
            picked = jnp.dot(chosen, results, preferred_element_type=jnp.float32)
            total = total + scale[:, choice : choice + 1] * picked
        return total

    own_in = sent_out(normal_rows, slot_ids)
    own_in, their_rows = lax.optimization_barrier((own_in, their_rows))
    their_in = sent_out(their_rows, their_slots)
    own_result = worked(own_in)
    own_result, their_in = lax.optimization_barrier((own_result, their_in))
    own_out = sent_back(own_result)
    own_out, their_result = lax.optimization_barrier((own_out, worked(their_in)))
    their_out = sent_back(their_result)
    their_sum = weighted(their_out, their_slots, their_weights).astype(jnp.bfloat16)
    returned = lax.ppermute(their_sum, "sp", across).astype(jnp.float32)
    combined = after_f + weighted(own_out, slot_ids, route_weights) + returned
    return combined.astype(jnp.bfloat16)


def solution(mesh):
    placed = (
        P(("sp", "tp"), None),
        P("sp", "tp"),
        P("sp", "tp"),
        P(None, "tp"),
        P("tp"),
        P("tp"),
        P("tp"),
        P(),
        P(),
        P(("sp", "tp"), None),
        P(("sp", "tp"), None),
        P("sp", None, "tp"),
        P("sp", None, "tp"),
        P("sp", "tp", None),
    )

    return jax.shard_map(
        on_device, mesh=mesh, in_specs=placed, out_specs=P(("sp", "tp"), None), check_vma=False
    )
```

```python
import functools

import jax
import jax.numpy as jnp
from jax import lax
from jax.experimental import pallas as pl
from jax.experimental.pallas import tpu as pltpu
from jax.sharding import PartitionSpec as P


def expert_body(count, own_steps, out_steps, rows, *refs):
    gates, uppers, downs = (refs[:count], refs[count : 2 * count], refs[2 * count : 3 * count])
    outs, hidden = (refs[3 * count : -1], refs[-1])
    step = pl.program_id(0)
    width = gates[0].shape[1]
    for part in range(count):

        @pl.when((step >= part * own_steps) & (step < (part + 1) * own_steps))
        def _(part=part):
            gate = jnp.dot(rows[...], gates[part][...], preferred_element_type=jnp.float32)
            upper = jnp.dot(rows[...], uppers[part][...], preferred_element_type=jnp.float32)
            value = (gate * jax.nn.sigmoid(gate) * upper).astype(jnp.bfloat16)
            hidden[step] = value

    first_steps = count * own_steps

    @pl.when(step >= first_steps)
    def _():
        total = None
        for part in range(count):
            for piece in range(own_steps):
                product = jnp.dot(
                    hidden[part * own_steps + piece],
                    downs[part][piece * width : (piece + 1) * width, :],
                    preferred_element_type=jnp.float32,
                )
                total = product if total is None else total + product
        each = out_steps // len(outs)
        for index, out in enumerate(outs):

            @pl.when((step - first_steps) // each == index)
            def _(out=out):
                out[...] = total.astype(jnp.bfloat16)


def expert_call(rows, gates, uppers, downs, parts):
    count = len(gates)
    row_total, model_width = rows.shape
    own_hidden = gates[0].shape[1]
    width = min(512, own_hidden)
    own_steps = own_hidden // width
    first_steps = count * own_steps
    out_steps = model_width // width
    each = out_steps // parts

    def inward(part):
        return pl.BlockSpec(
            (model_width, width),
            lambda i: (0, jnp.clip(i - part * own_steps, 0, own_steps - 1)),
        )

    outward = pl.BlockSpec(
        (own_hidden, width), lambda i: (0, jnp.clip(i - first_steps, 0, out_steps - 1))
    )
    return pl.pallas_call(
        functools.partial(expert_body, count, own_steps, out_steps),
        grid=(first_steps + out_steps,),
        in_specs=[pl.BlockSpec(memory_space=pltpu.VMEM)]
        + [inward(part) for part in range(count)] * 2
        + [outward] * count,
        out_specs=[
            pl.BlockSpec(
                (row_total, width),
                lambda i, part=part: (0, jnp.clip(i - first_steps - part * each, 0, each - 1)),
            )
            for part in range(parts)
        ],
        out_shape=[jax.ShapeDtypeStruct((row_total, model_width // parts), jnp.bfloat16)] * parts,
        scratch_shapes=[pltpu.VMEM((first_steps, row_total, width), jnp.bfloat16)],
        compiler_params=pltpu.CompilerParams(dimension_semantics=("arbitrary",)),
        cost_estimate=pl.CostEstimate(
            flops=6 * row_total * model_width * own_hidden * count,
            bytes_accessed=6 * model_width * own_hidden * count,
            transcendentals=row_total * own_hidden * count,
        ),
        name="expert_rows",
    )(pltpu.with_memory_space_constraint(rows, pltpu.VMEM), *gates, *uppers, *downs)


def prep_body(experts_all, slot_cap, *refs):
    values, gates, bias, gain, shift, ids, scales = refs[:7]
    last, vectors, packed, arrivals = refs[7:]
    lead = last.shape[0] // 2
    copies = []
    for index, source in enumerate((values, gates)):
        rows = pl.ds(source.shape[0] - lead, lead)
        copies.append(
            pltpu.make_async_copy(
                source.at[rows, :], last.at[pl.ds(index * lead, lead), :], arrivals.at[index]
            )
        )
    for copy in copies:
        copy.start()
    for index, source in enumerate((bias, gain, shift)):
        vectors[index : index + 1, :] = source[...]
    choose_count, row_count = ids.shape
    experts = lax.broadcasted_iota(jnp.int32, (experts_all, row_count), 0)
    named = [experts == ids[choice : choice + 1, :] for choice in range(choose_count)]
    marks = jnp.zeros((experts_all, row_count), jnp.float32)
    for mask in named:
        marks = jnp.where(mask, 1.0, marks)
    rows_down = lax.broadcasted_iota(jnp.int32, (row_count, row_count), 0)
    rows_along = lax.broadcasted_iota(jnp.int32, (row_count, row_count), 1)
    ahead = jnp.where(rows_down < rows_along, 1.0, 0.0).astype(jnp.bfloat16)
    before = jnp.dot(marks.astype(jnp.bfloat16), ahead, preferred_element_type=jnp.float32)
    packed[...] = jnp.zeros(packed.shape, jnp.float32)
    for choice, mask in enumerate(named):
        rank = jnp.sum(jnp.where(mask, before, 0.0), 0, keepdims=True)
        slot = ids[choice : choice + 1, :].astype(jnp.float32) * float(slot_cap) + rank
        packed[choice : choice + 1, :] = slot
        place = choose_count + choice
        packed[place : place + 1, :] = scales[choice : choice + 1, :]
    for copy in copies:
        copy.wait()


def prep_call(lead, experts_all, slot_cap, values, gates, vectors, ids, scales):
    choose_count, row_count = ids.shape
    width = values.shape[1]
    depth = -(-2 * choose_count // 8) * 8
    inside = pl.BlockSpec(memory_space=pltpu.VMEM)
    outside = pl.BlockSpec(memory_space=pl.ANY)
    return pl.pallas_call(
        functools.partial(prep_body, experts_all, slot_cap),
        in_specs=[outside, outside] + [inside] * 5,
        out_specs=[inside] * 3,
        out_shape=[
            jax.ShapeDtypeStruct((2 * lead, width), jnp.bfloat16),
            jax.ShapeDtypeStruct((len(vectors), width), jnp.float32),
            jax.ShapeDtypeStruct((depth, row_count), jnp.float32),
        ],
        scratch_shapes=[pltpu.SemaphoreType.DMA((2,))],
        name="prep_rows",
    )(values, gates, *[vector[None, :] for vector in vectors], ids, scales)


def front_body(taps_count, choose_count, count, lead, *refs):
    place = lax.axis_index("tp")
    values, gates, kernels, vectors, earlier = (
        refs[group * count : (group + 1) * count] for group in range(5)
    )
    slots, gain, residual_in, out_weight = refs[5 * count : 4 + 5 * count]
    after, normal, sendable = refs[4 + 5 * count : 7 + 5 * count]
    extended, taps, weight, residual, mixed, activated, arrivals = refs[7 + 5 * count :]
    fetch_weight = pltpu.make_async_copy(out_weight, weight, arrivals.at[0])
    fetch_residual = pltpu.make_async_copy(residual_in, residual, arrivals.at[1])
    fetch_weight.start()
    fetch_residual.start()
    row_count, chan_count = mixed.shape
    width = chan_count // count
    model_width = after.shape[1]
    lanes = min(128, width)
    piece = 32 if row_count % 32 == 0 else row_count

    def gated(value, gate):
        product = value.astype(jnp.float32) * jax.nn.sigmoid(gate.astype(jnp.float32))
        return product.astype(jnp.bfloat16).astype(jnp.float32)

    for member in range(count):

        @pl.when(place == member)
        def _(member=member):
            start = member * row_count
            for channel in range(count):
                shift = (member - channel) % count
                here = slice(channel * width, (channel + 1) * width)
                if member:
                    rows = slice(start - lead, start)
                    first = gated(values[shift][rows, :], gates[shift][rows, :])
                else:
                    first = gated(earlier[channel][:lead, :], earlier[channel][lead:, :])
                extended[:lead, here] = first
                rows = slice(start, start + row_count)
                extended[lead:, here] = gated(values[shift][rows, :], gates[shift][rows, :])
                taps[:taps_count, here] = kernels[shift][...]
                taps[taps_count:, here] = vectors[shift][...]

    origin = lead - (taps_count - 1)

    def convolve(index, carry):
        here = pl.ds(pl.multiple_of(index * lanes, lanes), lanes)
        total = jnp.zeros((row_count, lanes), jnp.float32) + taps[taps_count : taps_count + 1, here]
        for offset in range(min(8, taps_count)):
            used = range(offset, taps_count, 8)
            reach = row_count + 8 * (len(used) - 1)
            shifted = extended[origin + offset : origin + offset + reach, here]
            for turn, tap_index in enumerate(used):
                total = (
                    total
                    + taps[tap_index : tap_index + 1, here]
                    * shifted[8 * turn : 8 * turn + row_count]
                )
        mixed[:, here] = total
        return carry

    lax.fori_loop(0, chan_count // lanes, convolve, 0)
    scale = taps[taps_count + 1 : taps_count + 2, :]
    offset = taps[taps_count + 2 : taps_count + 3, :]

    def normalise(index, carry):
        here = pl.ds(pl.multiple_of(index * piece, piece), piece)
        held = mixed[here, :]
        center = jnp.sum(held, 1, keepdims=True) / chan_count
        spread = jnp.sum(held * held, 1, keepdims=True) / chan_count - center * center
        normed = (held - center) * lax.rsqrt(spread + 1e-06) * scale + offset
        activated[here, :] = (normed * jax.nn.sigmoid(normed)).astype(jnp.bfloat16)
        return carry

    lax.fori_loop(0, row_count // piece, normalise, 0)
    fetch_weight.wait()
    fetch_residual.wait()
    block = min(512, model_width)
    squares = jnp.zeros((row_count, 1), jnp.float32)
    for start in range(0, model_width, block):
        here = slice(start, start + block)
        product = jnp.dot(activated[...], weight[:, here], preferred_element_type=jnp.float32)
        rounded = (residual[:, here].astype(jnp.float32) + product).astype(jnp.bfloat16)
        after[:, here] = rounded
        again = rounded.astype(jnp.float32)
        squares = squares + jnp.sum(again * again, 1, keepdims=True)
    factor = lax.rsqrt(squares / model_width + 1e-06)
    local = sendable.shape[0]
    half = lax.axis_size("sp") // 2
    base = (lax.axis_index("sp") // half) * local
    positions = base + lax.broadcasted_iota(jnp.int32, (sendable.shape[0], row_count), 0)
    dispatch = jnp.zeros(positions.shape, jnp.float32)
    for choice in range(choose_count):
        slot = slots[choice : choice + 1, :].astype(jnp.int32)
        dispatch = jnp.where(positions == slot, 1.0, dispatch)
    dispatch = dispatch.astype(jnp.bfloat16)
    for start in range(0, model_width, block):
        here = slice(start, start + block)
        value = after[:, here].astype(jnp.float32) * factor * gain[:, here]
        value = value.astype(jnp.bfloat16)
        normal[:, here] = value
        picked = jnp.dot(dispatch, value, preferred_element_type=jnp.float32)
        sendable[:, here] = picked.astype(jnp.bfloat16)


def front_call(
    values,
    gates,
    kernels,
    vectors,
    earlier,
    slots,
    gain,
    residual_in,
    out_weight,
    local,
    choose_count,
):
    count = len(values)
    near = functools.partial(pltpu.with_memory_space_constraint, memory_space=pltpu.VMEM)
    row_count, model_width = residual_in.shape
    chan_count = out_weight.shape[0]
    taps_count = kernels[0].shape[0]
    lead = earlier[0].shape[0] // 2
    inside = pl.BlockSpec(memory_space=pltpu.VMEM)
    outside = pl.BlockSpec(memory_space=pl.ANY)
    result = jax.ShapeDtypeStruct((row_count, model_width), jnp.bfloat16)
    return pl.pallas_call(
        functools.partial(front_body, taps_count, choose_count, count, lead),
        in_specs=[inside] * (5 * count + 2) + [outside, outside],
        out_specs=[inside, inside, inside],
        out_shape=[result, result, jax.ShapeDtypeStruct((local, model_width), jnp.bfloat16)],
        scratch_shapes=[
            pltpu.VMEM((lead + row_count, chan_count), jnp.float32),
            pltpu.VMEM((taps_count + vectors[0].shape[0], chan_count), jnp.float32),
            pltpu.VMEM(out_weight.shape, jnp.bfloat16),
            pltpu.VMEM((row_count, model_width), jnp.bfloat16),
            pltpu.VMEM((row_count, chan_count), jnp.float32),
            pltpu.VMEM((row_count, chan_count), jnp.bfloat16),
            pltpu.SemaphoreType.DMA((2,)),
        ],
        cost_estimate=pl.CostEstimate(
            flops=2 * row_count * chan_count * (model_width + taps_count),
            bytes_accessed=2 * chan_count * model_width + 8 * row_count * model_width,
            transcendentals=2 * row_count * chan_count,
        ),
        name="front_rows",
    )(
        *values[:1],
        *[near(array) for array in values[1:]],
        *gates[:1],
        *[near(array) for array in gates[1:]],
        *kernels[:1],
        *[near(array) for array in kernels[1:]],
        *[near(array) for array in (*vectors, *earlier, slots)],
        gain,
        residual_in,
        out_weight,
    )


def on_device(
    residual_in,
    conv_values,
    conv_gates,
    conv_kernel,
    conv_bias,
    chan_gain,
    chan_shift,
    out_weight,
    norm_gain,
    route_ids,
    route_weights,
    expert_gate,
    expert_up,
    expert_down,
):
    taps_count = conv_kernel.shape[0]
    tok_count, _ = conv_values.shape
    tp_count = lax.axis_size("tp")
    row_count = tok_count // tp_count
    lead = -(-(taps_count - 1) // 16) * 16
    sp_count = lax.axis_size("sp")
    model_width = residual_in.shape[1]
    experts_all = expert_gate.shape[0] * sp_count
    choose_count = route_ids.shape[1]
    slot_cap = max(2, (2 * choose_count * row_count + experts_all - 1) // experts_all)
    last, vectors, packed = prep_call(
        lead,
        experts_all,
        slot_cap,
        conv_values,
        conv_gates,
        (conv_bias, chan_gain, chan_shift),
        route_ids.T,
        route_weights.T,
    )
    shared = [[conv_values], [conv_gates], [conv_kernel], [vectors]]
    for shift in range(1, tp_count):
        turn = [(source, (source + shift) % tp_count) for source in range(tp_count)]
        for held in shared:
            held.append(lax.ppermute(held[0], "tp", turn))
    earlier = []
    for channel in range(tp_count):
        pairs = [
            (source * tp_count + channel, (source + 1) * tp_count) for source in range(sp_count - 1)
        ]
        earlier.append(lax.ppermute(last, ("sp", "tp"), pairs))
    half = sp_count // 2
    local = half * slot_cap
    base = (lax.axis_index("sp") // half) * local
    across = [(source, (source + half) % sp_count) for source in range(sp_count)]
    groups = [list(range(start, start + half)) for start in range(0, sp_count, half)]
    exchange = functools.partial(
        lax.all_to_all,
        axis_name="sp",
        split_axis=0,
        concat_axis=0,
        tiled=True,
        axis_index_groups=groups,
    )
    after_mix, normal_rows, sendable = front_call(
        *shared,
        earlier,
        packed,
        norm_gain[None, :],
        residual_in,
        out_weight,
        local,
        choose_count,
    )
    after_f = after_mix.astype(jnp.float32)
    their_rows = lax.ppermute(normal_rows, "sp", across)
    packed, sendable = lax.optimization_barrier((packed, sendable))
    their_packed = lax.ppermute(packed, "sp", across)
    slot_ids = packed[:choose_count].astype(jnp.int32).T
    their_slots = their_packed[:choose_count].astype(jnp.int32)
    their_weights = their_packed[choose_count : 2 * choose_count].T
    held = (expert_gate[0], expert_up[0], expert_down[0])
    weights = [held]
    for shift in range(1, tp_count):
        turn = [(source, (source + shift) % tp_count) for source in range(tp_count)]
        weights.append(tuple(lax.ppermute(piece, "tp", turn) for piece in held))
    gates, uppers, downs = zip(*weights)

    def worked(rows, parts):
        return expert_call(rows.reshape(local, model_width), gates, uppers, downs, parts)

    def sent_back(rows):
        return exchange(rows.reshape(half, slot_cap, -1)).reshape(local, -1)

    def weighted(results, slots, scale):
        positions = base + lax.broadcasted_iota(jnp.int32, (1, local), 1)
        total = 0.0
        for choice in range(choose_count):
            chosen = (positions == slots[:, choice : choice + 1]).astype(jnp.bfloat16)
            picked = jnp.dot(chosen, results, preferred_element_type=jnp.float32)
            total = total + scale[:, choice : choice + 1] * picked
        return total

    own_in = exchange(sendable.reshape(half, slot_cap, model_width))
    positions = base + lax.broadcasted_iota(jnp.int32, (local, row_count), 0)
    marked = [positions == their_slots[k : k + 1] for k in range(choose_count)]
    dispatch = functools.reduce(jnp.logical_or, marked).astype(jnp.bfloat16)
    their_rows, own_in = lax.optimization_barrier((their_rows, own_in))
    their_send = jnp.dot(dispatch, their_rows, preferred_element_type=jnp.float32)
    their_send = their_send.astype(jnp.bfloat16).reshape(half, slot_cap, model_width)
    their_in = exchange(their_send)
    (own_result,) = worked(own_in, 1)
    own_result, their_in = lax.optimization_barrier((own_result, their_in))
    own_out = sent_back(own_result)
    their_parts = worked(their_in, 1)
    own_out, their_parts = lax.optimization_barrier((own_out, their_parts))
    own_sum = weighted(own_out, slot_ids, route_weights)
    their_out = sent_back(their_parts[0])
    their_sum = weighted(their_out, their_slots.T, their_weights).astype(jnp.bfloat16)
    returned = lax.ppermute(their_sum, "sp", across).astype(jnp.float32)
    combined = after_f + own_sum + returned
    return combined.astype(jnp.bfloat16)


def solution(mesh):
    placed = (
        P(("sp", "tp"), None),
        P("sp", "tp"),
        P("sp", "tp"),
        P(None, "tp"),
        P("tp"),
        P("tp"),
        P("tp"),
        P(),
        P(),
        P(("sp", "tp"), None),
        P(("sp", "tp"), None),
        P("sp", None, "tp"),
        P("sp", None, "tp"),
        P("sp", "tp", None),
    )

    return jax.shard_map(
        on_device, mesh=mesh, in_specs=placed, out_specs=P(("sp", "tp"), None), check_vma=False
    )
```

```python
import functools

import jax
import jax.numpy as jnp
from jax import lax
from jax.experimental import pallas as pl
from jax.experimental.pallas import tpu as pltpu
from jax.sharding import PartitionSpec as P


def expert_body(count, own_steps, out_steps, rows, *refs):
    gates, uppers, downs = (refs[:count], refs[count : 2 * count], refs[2 * count : 3 * count])
    outs, hidden = (refs[3 * count : -1], refs[-1])
    step = pl.program_id(0)
    width = gates[0].shape[1]
    for part in range(count):

        @pl.when((step >= part * own_steps) & (step < (part + 1) * own_steps))
        def _(part=part):
            gate = jnp.dot(rows[...], gates[part][...], preferred_element_type=jnp.float32)
            upper = jnp.dot(rows[...], uppers[part][...], preferred_element_type=jnp.float32)
            value = (gate * jax.nn.sigmoid(gate) * upper).astype(jnp.bfloat16)
            hidden[step] = value

    first_steps = count * own_steps

    @pl.when(step >= first_steps)
    def _():
        total = None
        for part in range(count):
            for piece in range(own_steps):
                product = jnp.dot(
                    hidden[part * own_steps + piece],
                    downs[part][piece * width : (piece + 1) * width, :],
                    preferred_element_type=jnp.float32,
                )
                total = product if total is None else total + product
        each = out_steps // len(outs)
        for index, out in enumerate(outs):

            @pl.when((step - first_steps) // each == index)
            def _(out=out):
                out[...] = total.astype(jnp.bfloat16)


def expert_call(rows, gates, uppers, downs, parts):
    count = len(gates)
    row_total, model_width = rows.shape
    own_hidden = gates[0].shape[1]
    width = min(512, own_hidden)
    own_steps = own_hidden // width
    first_steps = count * own_steps
    out_steps = model_width // width
    each = out_steps // parts

    def inward(part):
        return pl.BlockSpec(
            (model_width, width),
            lambda i: (0, jnp.clip(i - part * own_steps, 0, own_steps - 1)),
        )

    outward = pl.BlockSpec(
        (own_hidden, width), lambda i: (0, jnp.clip(i - first_steps, 0, out_steps - 1))
    )
    return pl.pallas_call(
        functools.partial(expert_body, count, own_steps, out_steps),
        grid=(first_steps + out_steps,),
        in_specs=[pl.BlockSpec(memory_space=pltpu.VMEM)]
        + [inward(part) for part in range(count)] * 2
        + [outward] * count,
        out_specs=[
            pl.BlockSpec(
                (row_total, width),
                lambda i, part=part: (0, jnp.clip(i - first_steps - part * each, 0, each - 1)),
            )
            for part in range(parts)
        ],
        out_shape=[jax.ShapeDtypeStruct((row_total, model_width // parts), jnp.bfloat16)] * parts,
        scratch_shapes=[pltpu.VMEM((first_steps, row_total, width), jnp.bfloat16)],
        compiler_params=pltpu.CompilerParams(dimension_semantics=("arbitrary",)),
        cost_estimate=pl.CostEstimate(
            flops=6 * row_total * model_width * own_hidden * count,
            bytes_accessed=6 * model_width * own_hidden * count,
            transcendentals=row_total * own_hidden * count,
        ),
        name="expert_rows",
    )(pltpu.with_memory_space_constraint(rows, pltpu.VMEM), *gates, *uppers, *downs)


def prep_body(experts_all, slot_cap, *refs):
    values, gates, bias, gain, shift, ids, scales = refs[:7]
    last, vectors, packed, arrivals = refs[7:]
    lead = last.shape[0] // 2
    copies = []
    for index, source in enumerate((values, gates)):
        rows = pl.ds(source.shape[0] - lead, lead)
        copies.append(
            pltpu.make_async_copy(
                source.at[rows, :], last.at[pl.ds(index * lead, lead), :], arrivals.at[index]
            )
        )
    for copy in copies:
        copy.start()
    for index, source in enumerate((bias, gain, shift)):
        vectors[index : index + 1, :] = source[...]
    choose_count, row_count = ids.shape
    experts = lax.broadcasted_iota(jnp.int32, (experts_all, row_count), 0)
    named = [experts == ids[choice : choice + 1, :] for choice in range(choose_count)]
    marks = jnp.zeros((experts_all, row_count), jnp.float32)
    for mask in named:
        marks = jnp.where(mask, 1.0, marks)
    rows_down = lax.broadcasted_iota(jnp.int32, (row_count, row_count), 0)
    rows_along = lax.broadcasted_iota(jnp.int32, (row_count, row_count), 1)
    ahead = jnp.where(rows_down < rows_along, 1.0, 0.0).astype(jnp.bfloat16)
    before = jnp.dot(marks.astype(jnp.bfloat16), ahead, preferred_element_type=jnp.float32)
    packed[...] = jnp.zeros(packed.shape, jnp.float32)
    for choice, mask in enumerate(named):
        rank = jnp.sum(jnp.where(mask, before, 0.0), 0, keepdims=True)
        slot = ids[choice : choice + 1, :].astype(jnp.float32) * float(slot_cap) + rank
        packed[choice : choice + 1, :] = slot
        place = choose_count + choice
        packed[place : place + 1, :] = scales[choice : choice + 1, :]
    for copy in copies:
        copy.wait()


def prep_call(lead, experts_all, slot_cap, values, gates, vectors, ids, scales):
    choose_count, row_count = ids.shape
    width = values.shape[1]
    depth = -(-2 * choose_count // 8) * 8
    inside = pl.BlockSpec(memory_space=pltpu.VMEM)
    outside = pl.BlockSpec(memory_space=pl.ANY)
    return pl.pallas_call(
        functools.partial(prep_body, experts_all, slot_cap),
        in_specs=[outside, outside] + [inside] * 5,
        out_specs=[inside] * 3,
        out_shape=[
            jax.ShapeDtypeStruct((2 * lead, width), jnp.bfloat16),
            jax.ShapeDtypeStruct((len(vectors), width), jnp.float32),
            jax.ShapeDtypeStruct((depth, row_count), jnp.float32),
        ],
        scratch_shapes=[pltpu.SemaphoreType.DMA((2,))],
        name="prep_rows",
    )(values, gates, *[vector[None, :] for vector in vectors], ids, scales)


def front_body(taps_count, choose_count, count, lead, *refs):
    place = lax.axis_index("tp")
    values, gates, kernels, vectors, earlier = (
        refs[group * count : (group + 1) * count] for group in range(5)
    )
    slots, gain, residual_in, out_weight = refs[5 * count : 4 + 5 * count]
    after, normal, sendable = refs[4 + 5 * count : 7 + 5 * count]
    extended, taps, weight, residual, mixed, activated, arrivals = refs[7 + 5 * count :]
    fetch_weight = pltpu.make_async_copy(out_weight, weight, arrivals.at[0])
    fetch_residual = pltpu.make_async_copy(residual_in, residual, arrivals.at[1])
    fetch_weight.start()
    fetch_residual.start()
    row_count, chan_count = mixed.shape
    width = chan_count // count
    model_width = after.shape[1]
    lanes = min(128, width)
    piece = 32 if row_count % 32 == 0 else row_count

    def gated(value, gate):
        product = value.astype(jnp.float32) * jax.nn.sigmoid(gate.astype(jnp.float32))
        return product.astype(jnp.bfloat16).astype(jnp.float32)

    for member in range(count):

        @pl.when(place == member)
        def _(member=member):
            start = member * row_count
            for channel in range(count):
                shift = (member - channel) % count
                here = slice(channel * width, (channel + 1) * width)
                if member:
                    rows = slice(start - lead, start)
                    first = gated(values[shift][rows, :], gates[shift][rows, :])
                else:
                    first = gated(earlier[channel][:lead, :], earlier[channel][lead:, :])
                extended[:lead, here] = first
                rows = slice(start, start + row_count)
                extended[lead:, here] = gated(values[shift][rows, :], gates[shift][rows, :])
                taps[:taps_count, here] = kernels[shift][...]
                taps[taps_count:, here] = vectors[shift][...]

    origin = lead - (taps_count - 1)

    def convolve(index, carry):
        here = pl.ds(pl.multiple_of(index * lanes, lanes), lanes)
        total = jnp.zeros((row_count, lanes), jnp.float32) + taps[taps_count : taps_count + 1, here]
        for offset in range(min(8, taps_count)):
            used = range(offset, taps_count, 8)
            reach = row_count + 8 * (len(used) - 1)
            shifted = extended[origin + offset : origin + offset + reach, here]
            for turn, tap_index in enumerate(used):
                total = (
                    total
                    + taps[tap_index : tap_index + 1, here]
                    * shifted[8 * turn : 8 * turn + row_count]
                )
        mixed[:, here] = total
        return carry

    lax.fori_loop(0, chan_count // lanes, convolve, 0)
    scale = taps[taps_count + 1 : taps_count + 2, :]
    offset = taps[taps_count + 2 : taps_count + 3, :]

    def normalise(index, carry):
        here = pl.ds(pl.multiple_of(index * piece, piece), piece)
        held = mixed[here, :]
        center = jnp.sum(held, 1, keepdims=True) / chan_count
        spread = jnp.sum(held * held, 1, keepdims=True) / chan_count - center * center
        normed = (held - center) * lax.rsqrt(spread + 1e-06) * scale + offset
        activated[here, :] = (normed * jax.nn.sigmoid(normed)).astype(jnp.bfloat16)
        return carry

    lax.fori_loop(0, row_count // piece, normalise, 0)
    fetch_weight.wait()
    fetch_residual.wait()
    block = min(512, model_width)
    squares = jnp.zeros((row_count, 1), jnp.float32)
    for start in range(0, model_width, block):
        here = slice(start, start + block)
        product = jnp.dot(activated[...], weight[:, here], preferred_element_type=jnp.float32)
        rounded = (residual[:, here].astype(jnp.float32) + product).astype(jnp.bfloat16)
        after[:, here] = rounded
        again = rounded.astype(jnp.float32)
        squares = squares + jnp.sum(again * again, 1, keepdims=True)
    factor = lax.rsqrt(squares / model_width + 1e-06)
    local = sendable.shape[0]
    half = lax.axis_size("sp") // 2
    base = (lax.axis_index("sp") // half) * local
    positions = base + lax.broadcasted_iota(jnp.int32, (sendable.shape[0], row_count), 0)
    dispatch = jnp.zeros(positions.shape, jnp.float32)
    for choice in range(choose_count):
        slot = slots[choice : choice + 1, :].astype(jnp.int32)
        dispatch = jnp.where(positions == slot, 1.0, dispatch)
    dispatch = dispatch.astype(jnp.bfloat16)
    for start in range(0, model_width, block):
        here = slice(start, start + block)
        value = after[:, here].astype(jnp.float32) * factor * gain[:, here]
        value = value.astype(jnp.bfloat16)
        normal[:, here] = value
        picked = jnp.dot(dispatch, value, preferred_element_type=jnp.float32)
        sendable[:, here] = picked.astype(jnp.bfloat16)


def front_call(
    values,
    gates,
    kernels,
    vectors,
    earlier,
    slots,
    gain,
    residual_in,
    out_weight,
    local,
    choose_count,
):
    count = len(values)
    near = functools.partial(pltpu.with_memory_space_constraint, memory_space=pltpu.VMEM)
    row_count, model_width = residual_in.shape
    chan_count = out_weight.shape[0]
    taps_count = kernels[0].shape[0]
    lead = earlier[0].shape[0] // 2
    inside = pl.BlockSpec(memory_space=pltpu.VMEM)
    outside = pl.BlockSpec(memory_space=pl.ANY)
    result = jax.ShapeDtypeStruct((row_count, model_width), jnp.bfloat16)
    return pl.pallas_call(
        functools.partial(front_body, taps_count, choose_count, count, lead),
        in_specs=[inside] * (5 * count + 2) + [outside, outside],
        out_specs=[inside, inside, inside],
        out_shape=[result, result, jax.ShapeDtypeStruct((local, model_width), jnp.bfloat16)],
        scratch_shapes=[
            pltpu.VMEM((lead + row_count, chan_count), jnp.float32),
            pltpu.VMEM((taps_count + vectors[0].shape[0], chan_count), jnp.float32),
            pltpu.VMEM(out_weight.shape, jnp.bfloat16),
            pltpu.VMEM((row_count, model_width), jnp.bfloat16),
            pltpu.VMEM((row_count, chan_count), jnp.float32),
            pltpu.VMEM((row_count, chan_count), jnp.bfloat16),
            pltpu.SemaphoreType.DMA((2,)),
        ],
        cost_estimate=pl.CostEstimate(
            flops=2 * row_count * chan_count * (model_width + taps_count),
            bytes_accessed=2 * chan_count * model_width + 8 * row_count * model_width,
            transcendentals=2 * row_count * chan_count,
        ),
        name="front_rows",
    )(
        *values[:1],
        *[near(array) for array in values[1:]],
        *gates[:1],
        *[near(array) for array in gates[1:]],
        *kernels[:1],
        *[near(array) for array in kernels[1:]],
        *vectors[:1],
        *[near(array) for array in (*vectors[1:], *earlier)],
        slots,
        gain,
        residual_in,
        out_weight,
    )


def on_device(
    residual_in,
    conv_values,
    conv_gates,
    conv_kernel,
    conv_bias,
    chan_gain,
    chan_shift,
    out_weight,
    norm_gain,
    route_ids,
    route_weights,
    expert_gate,
    expert_up,
    expert_down,
):
    taps_count = conv_kernel.shape[0]
    tok_count, _ = conv_values.shape
    tp_count = lax.axis_size("tp")
    row_count = tok_count // tp_count
    lead = -(-(taps_count - 1) // 16) * 16
    sp_count = lax.axis_size("sp")
    model_width = residual_in.shape[1]
    experts_all = expert_gate.shape[0] * sp_count
    choose_count = route_ids.shape[1]
    slot_cap = max(2, (2 * choose_count * row_count + experts_all - 1) // experts_all)
    last, vectors, packed = prep_call(
        lead,
        experts_all,
        slot_cap,
        conv_values,
        conv_gates,
        (conv_bias, chan_gain, chan_shift),
        route_ids.T,
        route_weights.T,
    )
    shared = [[conv_values], [conv_gates], [conv_kernel], [vectors]]
    for shift in range(1, tp_count):
        turn = [(source, (source + shift) % tp_count) for source in range(tp_count)]
        for held in shared:
            held.append(lax.ppermute(held[0], "tp", turn))
    earlier = []
    for channel in range(tp_count):
        pairs = [
            (source * tp_count + channel, (source + 1) * tp_count) for source in range(sp_count - 1)
        ]
        earlier.append(lax.ppermute(last, ("sp", "tp"), pairs))
    half = sp_count // 2
    local = half * slot_cap
    base = (lax.axis_index("sp") // half) * local
    across = [(source, (source + half) % sp_count) for source in range(sp_count)]
    groups = [list(range(start, start + half)) for start in range(0, sp_count, half)]
    exchange = functools.partial(
        lax.all_to_all,
        axis_name="sp",
        split_axis=0,
        concat_axis=0,
        tiled=True,
        axis_index_groups=groups,
    )
    after_mix, normal_rows, sendable = front_call(
        *shared,
        earlier,
        packed,
        norm_gain[None, :],
        residual_in,
        out_weight,
        local,
        choose_count,
    )
    after_f = after_mix.astype(jnp.float32)
    their_rows = lax.ppermute(normal_rows, "sp", across)
    packed, sendable = lax.optimization_barrier((packed, sendable))
    their_packed = lax.ppermute(packed, "sp", across)
    slot_ids = packed[:choose_count].astype(jnp.int32).T
    their_slots = their_packed[:choose_count].astype(jnp.int32)
    their_weights = their_packed[choose_count : 2 * choose_count].T
    held = (expert_gate[0], expert_up[0], expert_down[0])
    weights = [held]
    for shift in range(1, tp_count):
        turn = [(source, (source + shift) % tp_count) for source in range(tp_count)]
        weights.append(tuple(lax.ppermute(piece, "tp", turn) for piece in held))
    gates, uppers, downs = zip(*weights)

    def worked(rows, parts):
        return expert_call(rows.reshape(local, model_width), gates, uppers, downs, parts)

    def sent_back(rows):
        return exchange(rows.reshape(half, slot_cap, -1)).reshape(local, -1)

    def weighted(results, slots, scale):
        positions = base + lax.broadcasted_iota(jnp.int32, (1, local), 1)
        total = 0.0
        for choice in range(choose_count):
            chosen = (positions == slots[:, choice : choice + 1]).astype(jnp.bfloat16)
            picked = jnp.dot(chosen, results, preferred_element_type=jnp.float32)
            total = total + scale[:, choice : choice + 1] * picked
        return total

    own_in = exchange(sendable.reshape(half, slot_cap, model_width))
    positions = base + lax.broadcasted_iota(jnp.int32, (local, row_count), 0)
    marked = [positions == their_slots[k : k + 1] for k in range(choose_count)]
    dispatch = functools.reduce(jnp.logical_or, marked).astype(jnp.bfloat16)
    their_rows, own_in = lax.optimization_barrier((their_rows, own_in))
    their_send = jnp.dot(dispatch, their_rows, preferred_element_type=jnp.float32)
    their_send = their_send.astype(jnp.bfloat16).reshape(half, slot_cap, model_width)
    their_in = exchange(their_send)
    (own_result,) = worked(own_in, 1)
    own_result, their_in = lax.optimization_barrier((own_result, their_in))
    own_out = sent_back(own_result)
    their_parts = worked(their_in, 1)
    own_out, their_parts = lax.optimization_barrier((own_out, their_parts))
    own_sum = weighted(own_out, slot_ids, route_weights)
    their_out = sent_back(their_parts[0])
    their_sum = weighted(their_out, their_slots.T, their_weights).astype(jnp.bfloat16)
    returned = lax.ppermute(their_sum, "sp", across).astype(jnp.float32)
    settled = lax.optimization_barrier(after_f + own_sum)
    combined = settled + returned
    return combined.astype(jnp.bfloat16)


def solution(mesh):
    placed = (
        P(("sp", "tp"), None),
        P("sp", "tp"),
        P("sp", "tp"),
        P(None, "tp"),
        P("tp"),
        P("tp"),
        P("tp"),
        P(),
        P(),
        P(("sp", "tp"), None),
        P(("sp", "tp"), None),
        P("sp", None, "tp"),
        P("sp", None, "tp"),
        P("sp", "tp", None),
    )

    return jax.shard_map(
        on_device, mesh=mesh, in_specs=placed, out_specs=P(("sp", "tp"), None), check_vma=False
    )
```
